32 devices in a mesh: sp: 8 (over z, x), tp: 4 (over y, core).
Axes of the slice: x: 2, y: 2, z: 4, core: 2. Of those that a mesh axis runs over, the one named last changes fastest.
Arguments:
- broad_probe_tensor: bfloat16 [4096, 1024], P('sp', 'tp'), may hold values from -6 to 6
- broad_lookup_tensor: bfloat16 [4096, 1024], P('sp', 'tp'), may hold values from -6 to 6
- broad_payload_tensor: bfloat16 [4096, 1024], P('sp', 'tp'), may hold values from -6 to 6
- broad_emission_valve: bfloat16 [4096, 1024], P('sp', 'tp'), may hold values from -6 to 6
- slim_probe_tensor: bfloat16 [4096, 1024], P('sp', 'tp'), may hold values from -6 to 6
- slim_lookup_tensor: bfloat16 [4096, 1024], P('sp', 'tp'), may hold values from -6 to 6
- slim_payload_tensor: bfloat16 [4096, 1024], P('sp', 'tp'), may hold values from -6 to 6
- slim_emission_valve: bfloat16 [4096, 1024], P('sp', 'tp'), may hold values from -6 to 6
- broad_forgetting_speed: float32 [8], P('tp'), may hold values from -0.08 to 0
- slim_forgetting_speed: float32 [16], P('tp'), may hold values from -0.08 to 0
- broad_channel_scaling: float32 [1024], P('tp'), may hold values from 0.1 to 1.9
- slim_channel_scaling: float32 [1024], P('tp'), may hold values from 0.1 to 1.9
- surge_forgetting: float32 [4096], P('sp'), may hold values from -2.1 to 0
- broad_emission_proj: bfloat16 [1024, 2048], replicated, may hold values from -0.125 to 0.125
- slim_emission_proj: bfloat16 [1024, 2048], replicated, may hold values from -0.125 to 0.125
- skip_stream: bfloat16 [4096, 2048], P(('sp', 'tp')), may hold values from -6 to 6
- premix_scaling_coeffs: float32 [2048], replicated, may hold values from 0.1 to 1.9
- routed_specialist_ids: int32 [4096, 2], P('sp'), may hold values from 0 to 7, as said below
- routed_specialist_shares: float32 [4096, 2], P('sp'), may hold values from 0.2 to 1
- specialist_valve_proj: bfloat16 [8, 2048, 2048], P('sp', None, 'tp'), may hold values from -0.125 to 0.125
- specialist_expand_proj: bfloat16 [8, 2048, 2048], P('sp', None, 'tp'), may hold values from -0.125 to 0.125
- specialist_contract_proj: bfloat16 [8, 2048, 2048], P('sp', 'tp'), may hold values from -0.125 to 0.125
Outputs:
- result: bfloat16 [4096, 2048], P(('sp', 'tp'))
The draws below stay inside these ranges and needn't reach their ends.
Inputs may be any that keep to these rules, and one draw needn't show every extreme that they name: `routed_specialist_ids`: each row names two different experts of one group, that is of the same run of 2 consecutive experts. The rows of one device (each aligned block of 128 rows) name each expert at most 64 times, and some expert is named exactly 64 times by the rows of every device.
All inputs are finite; a program needn't handle non-finite values.
Results may differ from the reference program's by a relative error of at most 0.018.
Values may be sent and summed in bfloat16 or wider, within the bound.
No kernel may reach another device: no remote copies, remote signals or barrier semaphores. Data moves between devices by JAX's collectives and lax.ppermute only.
A program may use at most 128 MiB of HBM per device.

```python
import jax
import jax.numpy as jnp
from jax import lax

D = 2048
HA = 8
BROAD_CHANNEL_DIM = 128
HB = 16
THIN_CHANNEL_DIM = 64
FFE = 2048
GROUPS = 4
EXPERTS = 8
EXP_GROUP = 2
ROWS = 128
CAP = 64
TOKENS = 4096
BLOCK = 512
N_SP = 8
N_TP = 4


def rate_law(key, heads):
    pick_key, fast_key, slow_key = jax.random.split(key, 3)
    share = 5
    fast = jax.random.randint(pick_key, (heads,), 0, 10) < share
    span = jax.random.uniform(fast_key, (heads,), jnp.float32, 30.0, 100.0)
    slow = jnp.exp(jax.random.uniform(slow_key, (heads,), jnp.float32, jnp.log(0.02), jnp.log(0.2))) / TOKENS
    return jnp.where(fast, -jnp.log(10.0) / span, -slow).astype(jnp.float32)


def draw_broad_forgetting_speed(key, part):
    return rate_law(jax.random.fold_in(key, 11), HA)


def draw_slim_forgetting_speed(key, part):
    return rate_law(jax.random.fold_in(key, 12), HB)


def draw_surge_forgetting(key, part):
    where_key, size_key = jax.random.split(jax.random.fold_in(key, 21))
    spots = jax.random.randint(where_key, (3,), 0, TOKENS)
    kept = jax.random.uniform(size_key, (3,), jnp.float32, 0.5, 0.8)
    places = jnp.arange(TOKENS, dtype=jnp.int32)
    marks = jnp.where(places[None, :] == spots[:, None], jnp.log(kept)[:, None], 0.0)
    return jnp.sum(marks, 0).astype(jnp.float32)


def draw_routed_specialist_ids(key, part):
    base = jax.random.fold_in(key, 31)
    busy = jax.random.randint(jax.random.fold_in(base, 0), (), 0, GROUPS)
    blocks = TOKENS // ROWS
    units = CAP // 2

    def one(index):
        block_key = jax.random.fold_in(base, index + 1)
        cut_key, perm_key, offset_key, stride_key = jax.random.split(block_key, 4)
        cuts = jnp.sort(jax.random.randint(cut_key, (GROUPS - 2,), 0, units + 1))
        edges = jnp.concatenate([jnp.zeros((1,), jnp.int32), cuts, jnp.full((1,), units, jnp.int32)])
        counts = jnp.concatenate([jnp.full((1,), ROWS // 2, jnp.int32), (edges[1:] - edges[:-1]) * EXP_GROUP])
        ends = jnp.cumsum(counts)
        starts = ends - counts
        slot = jax.random.permutation(perm_key, ROWS)
        order = jnp.sum((slot[:, None] >= ends[None, :]).astype(jnp.int32), 1)
        inside = slot - starts[order]
        group = (busy + order) % GROUPS
        segment_begin = jax.random.randint(offset_key, (GROUPS,), 0, EXP_GROUP)
        stride = jax.random.randint(stride_key, (GROUPS,), 1, EXP_GROUP)
        first = group * EXP_GROUP + (segment_begin[group] + inside) % EXP_GROUP
        second = group * EXP_GROUP + (segment_begin[group] + inside + stride[group]) % EXP_GROUP
        return jnp.stack([first, second], 1)
    return jax.vmap(one)(jnp.arange(blocks, dtype=jnp.int32)).reshape(TOKENS, 2).astype(jnp.int32)


def steps_of(rng, dims, shards, smallest, largest):
    loudness = 1.0
    for position, parts in shards:
        heights = jax.random.uniform(jax.random.fold_in(jax.random.fold_in(rng, 6), position), (parts,), jnp.float32, smallest / len(shards), largest / len(shards))
        loudness = loudness * jnp.repeat(jnp.exp(heights), dims[position] // parts).reshape((-1,) + (1,) * (len(dims) - 1 - position))
    return loudness


def noise(stream_key, dims, scale, limit, cuts=(), kind=jnp.bfloat16):
    loudness = steps_of(stream_key, dims, cuts, -0.22, 0.18) if cuts else 1.0
    entries = jax.random.normal(stream_key, dims, jnp.float32) * scale * loudness
    return jnp.minimum(jnp.maximum(entries, -limit), limit).astype(kind)


def setup_inputs(seed: int = 0) -> dict:
    keys = jax.random.split(jax.random.key(seed), 23)
    return {
        "broad_probe_tensor": noise(keys[0], (TOKENS, HA * BROAD_CHANNEL_DIM), 1.0, 6.0, ((0, 8), (1, 4))),
        "broad_lookup_tensor": noise(keys[1], (TOKENS, HA * BROAD_CHANNEL_DIM), 1.0, 6.0, ((0, 8), (1, 4))),
        "broad_payload_tensor": noise(keys[2], (TOKENS, HA * BROAD_CHANNEL_DIM), 1.0, 6.0, ((0, 8), (1, 4))),
        "broad_emission_valve": noise(keys[3], (TOKENS, HA * BROAD_CHANNEL_DIM), 1.0, 6.0, ((0, 8), (1, 4))),
        "slim_probe_tensor": noise(keys[4], (TOKENS, HB * THIN_CHANNEL_DIM), 1.0, 6.0, ((0, 8), (1, 4))),
        "slim_lookup_tensor": noise(keys[5], (TOKENS, HB * THIN_CHANNEL_DIM), 1.0, 6.0, ((0, 8), (1, 4))),
        "slim_payload_tensor": noise(keys[6], (TOKENS, HB * THIN_CHANNEL_DIM), 1.0, 6.0, ((0, 8), (1, 4))),
        "slim_emission_valve": noise(keys[7], (TOKENS, HB * THIN_CHANNEL_DIM), 1.0, 6.0, ((0, 8), (1, 4))),
        "broad_forgetting_speed": draw_broad_forgetting_speed(jax.random.fold_in(keys[22], 71), 0),
        "slim_forgetting_speed": draw_slim_forgetting_speed(jax.random.fold_in(keys[22], 71), 0),
        "broad_channel_scaling": jnp.clip(1.0 + 0.18 * jax.random.normal(keys[10], (HA * BROAD_CHANNEL_DIM,), jnp.float32), 0.1, 1.9),
        "slim_channel_scaling": jnp.clip(1.0 + 0.18 * jax.random.normal(keys[11], (HB * THIN_CHANNEL_DIM,), jnp.float32), 0.1, 1.9),
        "surge_forgetting": draw_surge_forgetting(jax.random.fold_in(keys[22], 71), 0),
        "broad_emission_proj": noise(keys[13], (HA * BROAD_CHANNEL_DIM, D), (HA * BROAD_CHANNEL_DIM + HB * THIN_CHANNEL_DIM) ** -0.5, 0.125),
        "slim_emission_proj": noise(keys[14], (HB * THIN_CHANNEL_DIM, D), (HA * BROAD_CHANNEL_DIM + HB * THIN_CHANNEL_DIM) ** -0.5, 0.125),
        "skip_stream": noise(keys[15], (TOKENS, D), 1.0, 6.0, ((0, 32),)),
        "premix_scaling_coeffs": jnp.clip(1.0 + 0.18 * jax.random.normal(keys[16], (D,), jnp.float32), 0.1, 1.9),
        "routed_specialist_ids": draw_routed_specialist_ids(jax.random.fold_in(keys[22], 71), 0),
        "routed_specialist_shares": jnp.clip(0.2 + 0.8 * jax.random.uniform(keys[18], (TOKENS, 2), jnp.float32) ** steps_of(keys[18], (TOKENS, 2), ((0, 8),), -0.2, 0.2), 0.2, 1.0),
        "specialist_valve_proj": noise(keys[19], (EXPERTS, D, FFE), D ** -0.5, 0.125, ((0, 8), (2, 4))),
        "specialist_expand_proj": noise(keys[20], (EXPERTS, D, FFE), D ** -0.5, 0.125, ((0, 8), (2, 4))),
        "specialist_contract_proj": noise(keys[21], (EXPERTS, FFE, D), FFE ** -0.5, 0.125, ((0, 8), (1, 4))),
    }


rope_base = 10000.0
epsilon = 1e-06

def rotate(payload_tensor, positions):
    channel_dimension = payload_tensor.shape[-1]
    half = channel_dimension // 2
    freq = rope_base ** (-jnp.arange(half, dtype=jnp.float32) * 2.0 / channel_dimension)
    angle = positions.astype(jnp.float32)[:, None, None] * freq[None, None, :]
    cosine = jnp.cos(angle)
    sine = jnp.sin(angle)
    first = payload_tensor[..., :half]
    second = payload_tensor[..., half:]
    return jnp.concatenate([first * cosine - second * sine, first * sine + second * cosine], -1)

def prepare(probe_source, lookup_tensor, payload_tensor, heads, channel_dimension):
    length = probe_source.shape[0]
    places = jnp.arange(length, dtype=jnp.int32)
    spun_probe = rotate(probe_source.astype(jnp.float32).reshape(length, heads, channel_dimension), places).astype(jnp.bfloat16)
    spun_lookup = (rotate(lookup_tensor.astype(jnp.float32).reshape(length, heads, channel_dimension), places) * channel_dimension ** (-0.5)).astype(jnp.bfloat16)
    return (spun_probe, spun_lookup, payload_tensor.reshape(length, heads, channel_dimension))

def segment_terms(probe_tensor, lookup_tensor, payload_tensor, surge_forgetting, forgetting_speed):
    length = probe_tensor.shape[0]
    segment_tally = jnp.arange(length, dtype=jnp.float32)
    memory_matrix = forgetting_speed[None, :] * segment_tally[:, None] + jnp.cumsum(surge_forgetting)[:, None]
    causal = (segment_tally[:, None] >= segment_tally[None, :])[None]
    level_t = jnp.transpose(memory_matrix)
    gap = level_t[:, :, None] - level_t[:, None, :]
    decay = jnp.where(causal, jnp.exp(jnp.where(causal, gap, 0.0)), 0.0)
    attention_scores = jnp.einsum('szr,yzr->zsy', probe_tensor.astype(jnp.float32), lookup_tensor.astype(jnp.float32))
    weights = (attention_scores * decay).astype(jnp.bfloat16)
    inner = jnp.einsum('htm,mhe->the', weights.astype(jnp.float32), payload_tensor.astype(jnp.float32))
    factor = jnp.exp(memory_matrix + forgetting_speed[None, :])
    tail = jnp.exp(memory_matrix[-1:, :] - memory_matrix)
    weighted_output = (lookup_tensor.astype(jnp.float32) * tail[:, :, None]).astype(jnp.bfloat16)
    state_update = jnp.einsum('oup,our->upr', weighted_output.astype(jnp.float32), payload_tensor.astype(jnp.float32))
    total = jnp.exp(memory_matrix[-1] + forgetting_speed)
    return (inner, factor, state_update, total)

def read_state(probe_tensor, state):
    return jnp.einsum('thd,hde->the', probe_tensor.astype(jnp.float32), state, precision=lax.Precision.HIGHEST)

def finish(sublayer_final, emission_valve, scaling_coefficients):
    length, heads, channel_dimension = sublayer_final.shape
    normed = sublayer_final * lax.rsqrt(lax.optimization_barrier(jnp.mean(sublayer_final * sublayer_final, -1, keepdims=True)) + epsilon)
    gated = normed.reshape(length, heads * channel_dimension) * scaling_coefficients[None, :] * jax.nn.silu(emission_valve.astype(jnp.float32))
    return gated.astype(jnp.bfloat16)

def keeping_multiplier(probe_source, lookup_tensor, payload_tensor, emission_valve, forgetting_speed, scaling_coefficients, surge_forgetting, channel_dimension):
    heads = probe_source.shape[1] // channel_dimension
    spun_probe, spun_lookup, regrouped_payload = prepare(probe_source, lookup_tensor, payload_tensor, heads, channel_dimension)
    count = TOKENS // BLOCK

    def divider_mark(array):
        return array.reshape((count, BLOCK) + array.shape[1:])

    def segment_walker(state, piece):
        block_q, block_k, block_v, block_b = piece
        inner, factor, state_update, total = segment_terms(block_q, block_k, block_v, block_b, forgetting_speed)
        sublayer_final = inner + factor[:, :, None] * read_state(block_q, state)
        return (total[:, None, None] * state + state_update, sublayer_final)
    opening_location = jnp.zeros((heads, channel_dimension, channel_dimension), jnp.float32)
    ignored_placeholder, sublayer_final = lax.scan(segment_walker, opening_location, (divider_mark(spun_probe), divider_mark(spun_lookup), divider_mark(regrouped_payload), divider_mark(surge_forgetting)))
    return finish(sublayer_final.reshape(TOKENS, heads, channel_dimension), emission_valve, scaling_coefficients)

def experts_mix(normed, routed_specialist_ids, routed_specialist_shares, specialist_valve_proj, specialist_expand_proj, specialist_contract_proj):
    most = N_SP * N_TP * CAP
    slice_width = FFE // N_TP
    padded = jnp.concatenate([normed, jnp.zeros((1, D), jnp.bfloat16)], 0)

    def one(accum, index):
        matches = routed_specialist_ids == index
        weight = lax.optimization_barrier(jnp.sum(jnp.where(matches, routed_specialist_shares, 0.0), 1))
        weight = jnp.concatenate([weight, jnp.zeros((1,), jnp.float32)], 0)
        picked = jnp.nonzero(jnp.any(matches, 1), size=most, fill_value=TOKENS)[0].astype(jnp.int32)
        taken = padded[picked]
        emission_valve = jnp.dot(taken, specialist_valve_proj[index], preferred_element_type=jnp.float32)
        up = jnp.dot(taken, specialist_expand_proj[index], preferred_element_type=jnp.float32)
        hidden = (jax.nn.silu(emission_valve) * up).astype(jnp.bfloat16).reshape(most, N_TP, slice_width)
        down = specialist_contract_proj[index].reshape(N_TP, slice_width, D)
        partial_value = jnp.einsum('mpf,pfd->pmd', hidden.astype(jnp.float32), down.astype(jnp.float32))
        rounded = lax.optimization_barrier(partial_value.astype(jnp.bfloat16))
        expert_out = lax.optimization_barrier(jnp.sum(rounded.astype(jnp.float32), 0)).astype(jnp.bfloat16)
        accum = accum.at[picked].add(weight[picked][:, None] * expert_out.astype(jnp.float32))
        return (accum, None)
    opening_location = jnp.zeros((TOKENS + 1, D), jnp.float32)
    accum, ignored_placeholder = lax.scan(one, opening_location, jnp.arange(EXPERTS, dtype=jnp.int32))
    return accum[:TOKENS]

def reference(broad_probe_tensor, broad_lookup_tensor, broad_payload_tensor, broad_emission_valve, slim_probe_tensor, slim_lookup_tensor, slim_payload_tensor, slim_emission_valve, broad_forgetting_speed, slim_forgetting_speed, broad_channel_scaling, slim_channel_scaling, surge_forgetting, broad_emission_proj, slim_emission_proj, skip_stream, premix_scaling_coeffs, routed_specialist_ids, routed_specialist_shares, specialist_valve_proj, specialist_expand_proj, specialist_contract_proj):
    broad_channel_total = keeping_multiplier(broad_probe_tensor, broad_lookup_tensor, broad_payload_tensor, broad_emission_valve, broad_forgetting_speed, broad_channel_scaling, surge_forgetting, BROAD_CHANNEL_DIM)
    slim_channel_total = keeping_multiplier(slim_probe_tensor, slim_lookup_tensor, slim_payload_tensor, slim_emission_valve, slim_forgetting_speed, slim_channel_scaling, surge_forgetting, THIN_CHANNEL_DIM)
    projected = jnp.dot(broad_channel_total, broad_emission_proj, preferred_element_type=jnp.float32)
    projected = projected + jnp.dot(slim_channel_total, slim_emission_proj, preferred_element_type=jnp.float32)
    updated = skip_stream.astype(jnp.float32) + projected
    scale = lax.rsqrt(lax.optimization_barrier(jnp.mean(updated * updated, -1, keepdims=True)) + epsilon)
    normed = (updated * scale * premix_scaling_coeffs[None, :]).astype(jnp.bfloat16)
    mixture = experts_mix(normed, routed_specialist_ids, routed_specialist_shares, specialist_valve_proj, specialist_expand_proj, specialist_contract_proj)
    return (updated + mixture).astype(jnp.bfloat16)
```

```python
import functools

import jax
import jax.numpy as jnp
import numpy as np
from jax import lax
from jax.experimental import pallas as pl
from jax.experimental.pallas import tpu as pltpu
from jax.sharding import PartitionSpec as P

BROAD_CHANNEL_DIM = 128
THIN_CHANNEL_DIM = 64
GROUPS = 4


rope_base = 10000.0
epsilon = 1e-06


def entering(value, axis, join, neutral):
    place = lax.axis_index(axis)
    gathered = jax.tree.map(
        lambda a, kind: lax.all_gather(a.astype(kind), axis),
        value,
        (jnp.bfloat16, jnp.bfloat16, jnp.bfloat16, jnp.bfloat16),
    )
    state = jax.tree.map(lambda a, e: jnp.zeros_like(a) + jnp.asarray(e, a.dtype), value, neutral)

    def one(lap, state):
        return join(
            state,
            jax.tree.map(
                lambda a, own: lax.dynamic_index_in_dim(a, lap, 0, False).astype(own.dtype),
                gathered,
                value,
            ),
        )

    return lax.fori_loop(0, place, one, state)


def rotate(payload_tensor, positions):
    channel_dimension = payload_tensor.shape[-1]
    half = channel_dimension // 2
    freq = rope_base ** (-jnp.arange(half, dtype=jnp.float32) * 2.0 / channel_dimension)
    angle = positions.astype(jnp.float32)[:, None, None] * freq[None, None, :]
    cosine = jnp.cos(angle)
    sine = jnp.sin(angle)
    first = payload_tensor[..., :half]
    second = payload_tensor[..., half:]
    return jnp.concatenate([first * cosine - second * sine, first * sine + second * cosine], -1)


def segment_terms(probe_tensor, lookup_tensor, payload_tensor, surge_forgetting, forgetting_speed):
    length = probe_tensor.shape[0]
    segment_tally = jnp.arange(length, dtype=jnp.float32)
    memory_matrix = (
        forgetting_speed[None, :] * segment_tally[:, None] + jnp.cumsum(surge_forgetting)[:, None]
    )
    causal = (segment_tally[:, None] >= segment_tally[None, :])[None]
    level_t = jnp.transpose(memory_matrix)
    gap = level_t[:, :, None] - level_t[:, None, :]
    decay = jnp.where(causal, jnp.exp(jnp.where(causal, gap, 0.0)), 0.0)
    attention_scores = jnp.einsum(
        "szr,yzr->zsy", probe_tensor, lookup_tensor, preferred_element_type=jnp.float32
    )
    weights = (attention_scores * decay).astype(jnp.bfloat16)
    inner = jnp.einsum("htm,mhe->the", weights, payload_tensor, preferred_element_type=jnp.float32)
    factor = jnp.exp(memory_matrix + forgetting_speed[None, :])
    tail = jnp.exp(memory_matrix[-1:, :] - memory_matrix)
    weighted_output = (lookup_tensor.astype(jnp.float32) * tail[:, :, None]).astype(jnp.bfloat16)
    state_update = jnp.einsum(
        "oup,our->upr", weighted_output, payload_tensor, preferred_element_type=jnp.float32
    )
    total = jnp.exp(memory_matrix[-1] + forgetting_speed)
    return (inner, factor, state_update, total)


def read_state(probe_tensor, state):
    return jnp.einsum(
        "thd,hde->the", probe_tensor.astype(jnp.float32), state, precision=lax.Precision.HIGHEST
    )


def keeping_multiplier(
    probe_source,
    lookup_tensor,
    payload_tensor,
    forgetting_speed,
    surge_forgetting,
    channel_dimension,
    segment_begin,
):
    length = probe_source.shape[0]
    heads = probe_source.shape[1] // channel_dimension
    places = segment_begin + jnp.arange(length, dtype=jnp.int32)
    spun_probe = rotate(
        probe_source.astype(jnp.float32).reshape(length, heads, channel_dimension), places
    ).astype(jnp.bfloat16)
    spun_lookup = (
        rotate(lookup_tensor.astype(jnp.float32).reshape(length, heads, channel_dimension), places)
        * channel_dimension ** (-0.5)
    ).astype(jnp.bfloat16)
    regrouped_payload = payload_tensor.reshape(length, heads, channel_dimension)
    block = min(512, length)
    count = length // block

    def divider_mark(array):
        return array.reshape((count, block) + array.shape[1:])

    def segment_walker(carry, piece):
        state, prefix = carry
        block_q, block_k, block_v, block_b = piece
        inner, factor, state_update, total = segment_terms(
            block_q, block_k, block_v, block_b, forgetting_speed
        )
        local = inner + factor[:, :, None] * read_state(block_q, state)
        return (
            (total[:, None, None] * state + state_update, prefix * total),
            (local, factor * prefix[None, :]),
        )

    opening_location = (
        jnp.zeros((heads, channel_dimension, channel_dimension), jnp.float32),
        jnp.ones((heads,), jnp.float32),
    )
    (state, decay), (local, reach) = lax.scan(
        segment_walker,
        opening_location,
        (
            divider_mark(spun_probe),
            divider_mark(spun_lookup),
            divider_mark(regrouped_payload),
            divider_mark(surge_forgetting),
        ),
    )
    return (
        spun_probe,
        local.reshape(length, heads, channel_dimension),
        reach.reshape(length, heads),
        decay,
        state,
    )


def finish(sublayer_final, emission_valve, scaling_coefficients):
    length, heads, channel_dimension = sublayer_final.shape
    normed = sublayer_final * lax.rsqrt(
        jnp.mean(sublayer_final * sublayer_final, -1, keepdims=True) + epsilon
    )
    gated = (
        normed.reshape(length, heads * channel_dimension)
        * scaling_coefficients[None, :]
        * jax.nn.silu(emission_valve.astype(jnp.float32))
    )
    return gated.astype(jnp.bfloat16)


def chain(earlier, later):
    return (
        earlier[0] * later[0],
        later[0][:, None, None] * earlier[1] + later[1],
        earlier[2] * later[2],
        later[2][:, None, None] * earlier[3] + later[3],
    )


def slot_positions(chosen, experts, cap):
    listed = chosen.reshape(-1)
    matches = (listed[:, None] == jnp.arange(experts, dtype=jnp.int32)[None, :]).astype(jnp.int32)
    before = jnp.cumsum(matches, 0) - matches
    order = jnp.sum(before * matches, 1)
    return (listed * cap + order).reshape(chosen.shape)


def fill_slots(rows_in, chosen, experts, cap):
    count = rows_in.shape[0]
    places = slot_positions(chosen, experts, cap).reshape(-1)
    owners = jnp.repeat(jnp.arange(count, dtype=jnp.int32), 2)
    source = jnp.full((experts * cap,), count, jnp.int32).at[places].set(owners)
    padded = jnp.concatenate([rows_in, jnp.zeros((1, rows_in.shape[1]), rows_in.dtype)], 0)
    return padded[source].reshape(experts, cap, rows_in.shape[1])


def general_device(
    broad_probe_tensor,
    broad_lookup_tensor,
    broad_payload_tensor,
    broad_emission_valve,
    slim_probe_tensor,
    slim_lookup_tensor,
    slim_payload_tensor,
    slim_emission_valve,
    broad_forgetting_speed,
    slim_forgetting_speed,
    broad_channel_scaling,
    slim_channel_scaling,
    surge_forgetting,
    broad_emission_proj,
    slim_emission_proj,
    skip_stream,
    premix_scaling_coeffs,
    routed_specialist_ids,
    routed_specialist_shares,
    specialist_valve_proj,
    specialist_expand_proj,
    specialist_contract_proj,
):
    length = broad_probe_tensor.shape[0]
    segment_begin = lax.axis_index("sp") * length
    wide_result = keeping_multiplier(
        broad_probe_tensor,
        broad_lookup_tensor,
        broad_payload_tensor,
        broad_forgetting_speed,
        surge_forgetting,
        BROAD_CHANNEL_DIM,
        segment_begin,
    )
    narrow_result = keeping_multiplier(
        slim_probe_tensor,
        slim_lookup_tensor,
        slim_payload_tensor,
        slim_forgetting_speed,
        surge_forgetting,
        THIN_CHANNEL_DIM,
        segment_begin,
    )
    identity = (
        jnp.ones_like(wide_result[3]),
        jnp.zeros_like(wide_result[4]),
        jnp.ones_like(narrow_result[3]),
        jnp.zeros_like(narrow_result[4]),
    )
    incoming = entering(
        (wide_result[3], wide_result[4], narrow_result[3], narrow_result[4]), "sp", chain, identity
    )
    mixed_wide = finish(
        wide_result[1] + wide_result[2][:, :, None] * read_state(wide_result[0], incoming[1]),
        broad_emission_valve,
        broad_channel_scaling,
    )
    mixed_narrow = finish(
        narrow_result[1] + narrow_result[2][:, :, None] * read_state(narrow_result[0], incoming[3]),
        slim_emission_valve,
        slim_channel_scaling,
    )
    rows_wide, rows_narrow = (
        lax.all_to_all(mixed_wide, "tp", split_axis=0, concat_axis=1, tiled=True),
        lax.all_to_all(mixed_narrow, "tp", split_axis=0, concat_axis=1, tiled=True),
    )
    projected = jnp.dot(rows_wide, broad_emission_proj, preferred_element_type=jnp.float32)
    projected = projected + jnp.dot(
        rows_narrow, slim_emission_proj, preferred_element_type=jnp.float32
    )
    updated = skip_stream.astype(jnp.float32) + projected
    scale = lax.rsqrt(jnp.mean(updated * updated, -1, keepdims=True) + epsilon)
    normed = (updated * scale * premix_scaling_coeffs[None, :]).astype(jnp.bfloat16)
    rows = normed.shape[0]
    width = normed.shape[1]
    experts = lax.axis_size("sp") * specialist_valve_proj.shape[0]
    cap = rows * GROUPS // experts
    own_ids = lax.dynamic_slice_in_dim(routed_specialist_ids, lax.axis_index("tp") * rows, rows, 0)
    own_weights = lax.dynamic_slice_in_dim(
        routed_specialist_shares, lax.axis_index("tp") * rows, rows, 0
    )
    own_places = slot_positions(own_ids, experts, cap)
    sent = lax.all_to_all(
        fill_slots(normed, own_ids, experts, cap), "sp", split_axis=0, concat_axis=0, tiled=True
    )
    arrived = lax.all_gather(sent, "tp", axis=0, tiled=True)
    slots = arrived.reshape(-1, width)
    emission_valve = jnp.dot(slots, specialist_valve_proj[0], preferred_element_type=jnp.float32)
    up = jnp.dot(slots, specialist_expand_proj[0], preferred_element_type=jnp.float32)
    hidden = (jax.nn.silu(emission_valve) * up).astype(jnp.bfloat16)
    summed = lax.psum_scatter(
        jnp.dot(hidden, specialist_contract_proj[0], preferred_element_type=jnp.float32).astype(
            jnp.bfloat16
        ),
        "tp",
        scatter_dimension=0,
        tiled=True,
    )
    expert_out = summed.reshape(experts, cap, width)
    returned = lax.all_to_all(expert_out, "sp", split_axis=0, concat_axis=0, tiled=True)
    picked = returned.reshape(experts * cap, width)[own_places]
    mixture = jnp.sum(own_weights[:, :, None] * picked.astype(jnp.float32), 1)
    return (updated + mixture).astype(jnp.bfloat16)


LANES = 128
NOTES = 128
CHUNKS = 2
F32 = jnp.float32
BF16 = jnp.bfloat16


def rope_tables(length, blocks):
    def lanes(dim):
        lane = np.arange(LANES) % dim
        freq = rope_base ** (-(lane % (dim // 2)) * 2.0 / dim)
        sign = np.where(lane < dim // 2, -1.0, 1.0)
        return freq, sign

    inside, starts = [], []
    for dim in (BROAD_CHANNEL_DIM, THIN_CHANNEL_DIM):
        freq, sign = lanes(dim)
        for rows, step, into in ((length, 1, inside), (blocks, length, starts)):
            angle = np.arange(rows)[:, None] * step * freq[None, :]
            into += [np.cos(angle), np.sin(angle) * sign]
    return np.stack(inside).astype(np.float32), np.stack(starts).astype(np.float32)


def turning(tables_ref, starts_ref, sp_index, group):
    ci, si = tables_ref[2 * group], tables_ref[2 * group + 1]
    cb = starts_ref[2 * group, pl.ds(sp_index, 1), :]
    sb = starts_ref[2 * group + 1, pl.ds(sp_index, 1), :]
    return ci * cb - si * sb, si * cb + ci * sb


def swap_halves(x, group):
    if group == 0:
        return pltpu.roll(x, 64, 1)
    lane = lax.broadcasted_iota(jnp.int32, x.shape, 1)
    return jnp.where(lane % 64 < 32, pltpu.roll(x, 96, 1), pltpu.roll(x, 32, 1))


def running_sum(surge_ref):
    length = surge_ref.shape[1]
    row = jnp.broadcast_to(surge_ref[...], (8, length))
    lane = lax.broadcasted_iota(jnp.int32, row.shape, 1)
    step = 1
    while step < length:
        row = row + jnp.where(lane >= step, pltpu.roll(row, step, 1), 0.0)
        step *= 2
    return row[0:1, :]


def as_column(row):
    length = row.shape[1]
    t = lax.broadcasted_iota(jnp.int32, (length, length), 0)
    m = lax.broadcasted_iota(jnp.int32, (length, length), 1)
    return jnp.sum(jnp.where(t == m, row, jnp.zeros_like(row)), axis=1, keepdims=True)


def low_half(shape):
    return lax.broadcasted_iota(jnp.int32, shape, 1) < 64


def dot(a, b, dims=((1,), (0,))):
    return lax.dot_general(a, b, (dims, ((), ())), preferred_element_type=F32)


def increment_kernel(
    where_ref, wide_rate, slim_rate, surge_ref, tables_ref, starts_ref,
    kw_ref, vw_ref, kn_ref, vn_ref,
    kw_out, kn_out, message_ref,
):
    length = kw_ref.shape[0]
    row = running_sum(surge_ref)
    column = as_column(row)
    last = row[0:1, length - 1 : length]
    offset = lax.broadcasted_iota(jnp.int32, (length, 1), 0).astype(F32)
    back = (length - 1.0) - offset
    below = last - column
    half = low_half((1, LANES))
    decays = []
    for group, (k_ref, v_ref, k_out, rates) in enumerate(
        ((kw_ref, vw_ref, kw_out, wide_rate), (kn_ref, vn_ref, kn_out, slim_rate))
    ):
        cosine, sine = turning(tables_ref, starts_ref, where_ref[0], group)
        scale = (BROAD_CHANNEL_DIM, THIN_CHANNEL_DIM)[group] ** -0.5
        for slot in range(2):
            cols = slice(slot * LANES, (slot + 1) * LANES)
            k = k_ref[:, cols].astype(F32)
            spun = ((k * cosine + swap_halves(k, group) * sine) * scale).astype(BF16)
            k_out[:, cols] = spun
            if group == 0:
                tail = jnp.exp(rates[slot] * back + below)
                decay = jnp.exp(jnp.full((1, LANES), rates[slot] * length) + last)
            else:
                a, b = rates[2 * slot], rates[2 * slot + 1]
                tail = jnp.where(half, jnp.exp(a * back + below), jnp.exp(b * back + below))
                decay = jnp.exp(jnp.where(half, a * length, b * length) + last)
            weighted = (spun.astype(F32) * tail).astype(BF16)
            gain = dot(weighted, v_ref[:, cols], ((0,), (0,)))
            if group == 1:
                upper = lax.broadcasted_iota(jnp.int32, (LANES, LANES), 0) < 64
                gain = jnp.where(upper == low_half((LANES, LANES)), gain, 0.0)
            place = (2 * group + slot) * LANES
            message_ref[place : place + LANES, :] = gain.astype(BF16)
            decays.append(decay)
    high = [d.astype(BF16).astype(F32) for d in decays]
    low = [d - h for d, h in zip(decays, high)]
    notes = jnp.concatenate(high + low + [jnp.zeros((8, LANES), F32)], 0)
    message_ref[4 * LANES :, :] = notes.astype(BF16)


def unpack(ref):
    notes = ref[4 * LANES :, :].astype(F32)
    decays = [notes[i : i + 1] + notes[i + 4 : i + 5] for i in range(4)]
    states = [ref[i * LANES : (i + 1) * LANES, :].astype(F32) for i in range(4)]
    return states, decays


def pair_kernel(where_ref, own_ref, other_ref, out_ref):
    late = where_ref[2] == 1
    own, own_decay = unpack(own_ref)
    other, other_decay = unpack(other_ref)
    high, low = [], []
    for i in range(4):
        first = jnp.where(late, other[i], own[i])
        second = jnp.where(late, own[i], other[i])
        decay = jnp.where(late, own_decay[i], other_decay[i])
        out_ref[i * LANES : (i + 1) * LANES, :] = (decay * first + second).astype(BF16)
        both = own_decay[i] * other_decay[i]
        high.append(both.astype(BF16).astype(F32))
        low.append(both - high[-1])
    notes = jnp.concatenate(high + low + [jnp.zeros((8, LANES), F32)], 0)
    out_ref[4 * LANES :, :] = notes.astype(BF16)


def inner_kernel(
    where_ref, wide_rate, slim_rate, surge_ref, tables_ref, starts_ref,
    qw_ref, kw_ref, vw_ref, qn_ref, kn_ref, vn_ref,
    q_out, inner_out, column_out,
):
    length = qw_ref.shape[0]
    row = running_sum(surge_ref)
    column = as_column(row)
    column_out[...] = jnp.broadcast_to(column, (length, LANES))
    for group, q_ref in enumerate((qw_ref, qn_ref)):
        cosine, sine = turning(tables_ref, starts_ref, where_ref[0], group)
        for slot in range(2):
            cols = slice(slot * LANES, (slot + 1) * LANES)
            q = q_ref[:, cols].astype(F32)
            place = (2 * group + slot) * LANES
            q_out[:, place : place + LANES] = (
                q * cosine + swap_halves(q, group) * sine
            ).astype(BF16)
    tile = min(128, length)
    half = low_half((tile, LANES))
    for block in range(length // tile):
        begin, n = block * tile, (block + 1) * tile
        rows = slice(begin, n)
        t = lax.broadcasted_iota(jnp.int32, (tile, n), 0) + begin
        m = lax.broadcasted_iota(jnp.int32, (tile, n), 1)
        causal = t >= m
        apart = (t - m).astype(F32)
        fall = column[rows] - row[:, :n]

        def mixed(q, k, v, rate):
            decay = jnp.where(causal, jnp.exp(rate * apart + fall), 0.0)
            return dot((dot(q, k, ((1,), (1,))) * decay).astype(BF16), v)

        for slot in range(2):
            cols = slice(slot * LANES, (slot + 1) * LANES)
            q = q_out[rows, cols]
            inner_out[rows, cols] = mixed(q, kw_ref[:n, cols], vw_ref[:n, cols], wide_rate[slot])
            place = slice((2 + slot) * LANES, (3 + slot) * LANES)
            q = q_out[rows, place]
            k, v = kn_ref[:n, cols], vn_ref[:n, cols]
            nothing = jnp.zeros_like(q)
            first = mixed(jnp.where(half, q, nothing), k, v, slim_rate[2 * slot])
            second = mixed(jnp.where(half, nothing, q), k, v, slim_rate[2 * slot + 1])
            inner_out[rows, place] = jnp.where(half, first, second)


def finish_kernel(
    where_ref, wide_rate, slim_rate, column_ref, q_ref, inner_ref,
    other_ref, near_ref, mid_ref, far_ref,
    wide_gate, slim_gate, wide_gain, slim_gain,
    *outs,
):
    late = where_ref[2] == 1
    tp_index = where_ref[3]
    rows = outs[0].shape[0]
    near, near_decay = unpack(near_ref)
    mid, mid_decay = unpack(mid_ref)
    far, _ = unpack(far_ref)
    other, other_decay = unpack(other_ref)
    states = []
    for i in range(4):
        state = near[i] + near_decay[i] * (mid[i] + mid_decay[i] * far[i])
        state = jnp.where(late, other_decay[i] * state + other[i], state)
        high = state.astype(BF16)
        states.append((high, (state - high.astype(F32)).astype(BF16)))
    half = low_half((rows, LANES))
    for hop, out in enumerate(outs):
        begin = pl.multiple_of((tp_index ^ hop) * rows, rows)
        at = pl.ds(begin, rows)
        column = column_ref[at, :]
        offset = (lax.broadcasted_iota(jnp.int32, (rows, LANES), 0) + begin + 1).astype(F32)
        for i in range(4):
            cols = slice(i * LANES, (i + 1) * LANES)
            q = q_ref[at, cols]
            read = dot(q, states[i][0]) + dot(q, states[i][1])
            if i < 2:
                factor = jnp.exp(wide_rate[i] * offset + column)
                gate_ref, gain_ref = wide_gate, wide_gain
            else:
                rate = jnp.where(half, slim_rate[2 * i - 4], slim_rate[2 * i - 3])
                factor = jnp.exp(rate * offset + column)
                gate_ref, gain_ref = slim_gate, slim_gain
            value = inner_ref[at, cols] + factor * read
            square = value * value
            if i < 2:
                mean = jnp.mean(square, axis=1, keepdims=True)
            else:
                first = jnp.sum(jnp.where(half, square, 0.0), axis=1, keepdims=True)
                second = jnp.sum(jnp.where(half, 0.0, square), axis=1, keepdims=True)
                mean = jnp.where(half, first, second) / THIN_CHANNEL_DIM
            part = slice((i % 2) * LANES, (i % 2 + 1) * LANES)
            gate = gate_ref[at, part].astype(F32)
            value = value * lax.rsqrt(mean + epsilon) * gain_ref[:, part]
            out[:, cols] = (value * (gate / (1.0 + jnp.exp(-gate)))).astype(BF16)


def project_kernel(
    where_ref, p0, p1, p2, p3, wide_ref, slim_ref, skip_ref, gain_ref, ids_ref, shares_ref,
    updated_ref, pick_ref, *rest,
):
    outs, acc = rest[:-1], rest[-1]
    step = pl.program_id(0)
    width = wide_ref.shape[0]

    for hop, piece in enumerate((p0, p1, p2, p3)):

        @pl.when(step == hop)
        def _(hop=hop, piece=piece):
            part = dot(piece[:, :width], wide_ref[...]) + dot(piece[:, width:], slim_ref[...])
            if hop == 0:
                acc[...] = skip_ref[...].astype(F32) + part
            else:
                acc[...] += part

    @pl.when(step == 3)
    def _():
        updated = acc[...]
        updated_ref[...] = updated
        rows = updated.shape[0]
        scale = lax.rsqrt(jnp.mean(updated * updated, axis=1, keepdims=True) + epsilon)
        normed = (updated * scale * gain_ref[...]).astype(BF16)
        ids, shares = ids_ref[...], shares_ref[...]
        first, second = ids[:, 0:1], ids[:, 1:2]
        group = first // 2
        straight = first < second
        low = jnp.where(straight, shares[:, 0:1], shares[:, 1:2])
        high = jnp.where(straight, shares[:, 1:2], shares[:, 0:1])
        lane = lax.broadcasted_iota(jnp.int32, (rows, NOTES), 1)
        share = jnp.where(lane < 2, low, high)
        top = share.astype(BF16).astype(F32)
        notes = jnp.where(lane % 2 == 0, top, share - top).astype(BF16)
        t = lax.broadcasted_iota(jnp.int32, (rows, rows), 0)
        m = lax.broadcasted_iota(jnp.int32, (rows, rows), 1)
        group_f = jnp.broadcast_to(group.astype(F32), (rows, rows))
        across = jnp.sum(jnp.where(t == m, group_f, 0.0), axis=0, keepdims=True)
        ahead = jnp.where((group_f == across) & (t < m), 1.0, 0.0)
        order = jnp.sum(ahead, axis=0, keepdims=True).astype(jnp.int32)
        across = across.astype(jnp.int32)
        cap = pick_ref.shape[0] // GROUPS
        each = outs[0].shape[0]
        slot = lax.broadcasted_iota(jnp.int32, (cap, rows), 0)
        for hop in range(GROUPS):
            aim = (where_ref[1] + hop) % GROUPS
            pick = jnp.where((order == slot) & (across == aim), 1.0, 0.0).astype(BF16)
            pick_ref[hop * cap : (hop + 1) * cap, :] = pick
            body = dot(pick, normed).astype(BF16)
            side = dot(pick, notes).astype(BF16)
            for chunk in range(cap // each):
                out = outs[chunk * GROUPS + hop]
                out[:, : normed.shape[1]] = body[chunk * each : (chunk + 1) * each]
                out[:, normed.shape[1] :] = side[chunk * each : (chunk + 1) * each]


def expert_kernel(count, where_ref, *refs):
    blocks = refs[:count]
    weights = refs[count : count + 6]
    outs = refs[count + 6 : 2 * count + 6]
    gate_buf, up_buf, down_buf, acc, sems = refs[2 * count + 6 :]
    steps, model, tile = gate_buf.shape
    each = steps // 2

    def copies(step):
        side, cut = divmod(step, each)
        span = slice(cut * tile, (cut + 1) * tile)
        gate, up, down = weights[side], weights[2 + side], weights[4 + side]
        return (
            pltpu.make_async_copy(gate.at[0, :, span], gate_buf.at[step], sems.at[step, 0]),
            pltpu.make_async_copy(up.at[0, :, span], up_buf.at[step], sems.at[step, 1]),
            pltpu.make_async_copy(down.at[0, span, :], down_buf.at[step], sems.at[step, 2]),
        )

    for step in range(steps):
        for copy in copies(step):
            copy.start()
    late = where_ref[2] == 1
    for step in range(steps):
        for copy in copies(step):
            copy.wait()
        for i, block in enumerate(blocks):
            x = block[:, :model]
            gate = dot(x, gate_buf[step])
            up = dot(x, up_buf[step])
            hidden = (gate / (1.0 + jnp.exp(-gate)) * up).astype(BF16)
            part = dot(hidden, down_buf[step])
            if step == 0:
                acc[i] = part
            else:
                acc[i] += part
    for i, block in enumerate(blocks):
        notes = block[:, model : model + 4].astype(F32)
        share = jnp.where(late, notes[:, 2:3] + notes[:, 3:4], notes[:, 0:1] + notes[:, 1:2])
        outs[i][...] = (acc[i] * share).astype(BF16)


def combine_kernel(updated_ref, pick_ref, *refs):
    parts, out = refs[:-1], refs[-1]
    each = parts[0].shape[0]
    cap = pick_ref.shape[0] // GROUPS
    total = updated_ref[...]
    for hop in range(GROUPS):
        for chunk in range(cap // each):
            place = hop * cap + chunk * each
            pick = pick_ref[place : place + each, :]
            total = total + dot(pick, parts[chunk * GROUPS + hop][...], ((0,), (0,)))
    out[...] = total.astype(BF16)


SMEM = pl.BlockSpec(memory_space=pltpu.SMEM)
VMEM = pl.BlockSpec(memory_space=pltpu.VMEM)
ANY = pl.BlockSpec(memory_space=pl.ANY)
BIG = pltpu.CompilerParams(vmem_limit_bytes=48 * 1024 * 1024)


def call(kernel, name, outs, specs, scratch=()):
    shapes = [jax.ShapeDtypeStruct(s, d) for s, d in outs]
    return pl.pallas_call(
        kernel,
        out_shape=shapes,
        in_specs=specs,
        out_specs=[VMEM] * len(shapes),
        scratch_shapes=list(scratch),
        compiler_params=BIG,
        name=name,
    )


def paired_device(
    blocks,
    broad_probe_tensor,
    broad_lookup_tensor,
    broad_payload_tensor,
    broad_emission_valve,
    slim_probe_tensor,
    slim_lookup_tensor,
    slim_payload_tensor,
    slim_emission_valve,
    broad_forgetting_speed,
    slim_forgetting_speed,
    broad_channel_scaling,
    slim_channel_scaling,
    surge_forgetting,
    broad_emission_proj,
    slim_emission_proj,
    skip_stream,
    premix_scaling_coeffs,
    routed_specialist_ids,
    routed_specialist_shares,
    specialist_valve_proj,
    specialist_expand_proj,
    specialist_contract_proj,
):
    length, width = broad_probe_tensor.shape
    rows, model = skip_stream.shape
    sp_index, tp_index = lax.axis_index("sp"), lax.axis_index("tp")
    where = jnp.stack([sp_index, sp_index // 2, sp_index % 2, tp_index]).astype(jnp.int32)

    def swap_expert(a):
        return lax.ppermute(a, "sp", [(i, i ^ 1) for i in range(blocks)])

    def swap_rows(a, hop):
        return lax.ppermute(a, "tp", [(i, i ^ hop) for i in range(4)])

    def turn_groups(a, hop):
        return lax.ppermute(a, "sp", [(i, (i + 2 * hop) % blocks) for i in range(blocks)])

    def pass_on(a, hop):
        return lax.ppermute(a, "sp", [(i, i + 2 * hop) for i in range(blocks - 2 * hop)])

    sides = []
    for w in (specialist_valve_proj, specialist_expand_proj, specialist_contract_proj):
        sides += [w, swap_rows(w, 1)]

    inside, starts = rope_tables(length, blocks)
    inside, starts = jnp.asarray(inside), jnp.asarray(starts)
    surge = surge_forgetting.reshape(1, length)
    rates = (broad_forgetting_speed, slim_forgetting_speed)
    spun_wide, spun_slim, message = call(
        increment_kernel,
        "increment",
        [((length, width), BF16), ((length, width), BF16), ((4 * LANES + 16, LANES), BF16)],
        [SMEM] * 3 + [VMEM] * 7,
    )(
        where, *rates, surge, inside, starts,
        broad_lookup_tensor, broad_payload_tensor, slim_lookup_tensor, slim_payload_tensor,
    )
    other = swap_expert(message)
    pair = call(pair_kernel, "pair", [(message.shape, BF16)], [SMEM] + [VMEM] * 2)(
        where, message, other
    )[0]
    passed = [pass_on(pair, hop) for hop in range(1, GROUPS)]
    spun_probe, inner, column = call(
        inner_kernel,
        "inner",
        [((length, 2 * width), BF16), ((length, 2 * width), F32), ((length, LANES), F32)],
        [SMEM] * 3 + [VMEM] * 9,
    )(
        where, *rates, surge, inside, starts,
        broad_probe_tensor, spun_wide, broad_payload_tensor,
        slim_probe_tensor, spun_slim, slim_payload_tensor,
    )
    pieces = call(
        finish_kernel, "finish", [((rows, 2 * width), BF16)] * 4, [SMEM] * 3 + [VMEM] * 11
    )(
        where, *rates, column, spun_probe, inner, other, *passed,
        broad_emission_valve, slim_emission_valve,
        broad_channel_scaling.reshape(1, width), slim_channel_scaling.reshape(1, width),
    )
    pieces = [pieces[0]] + [swap_rows(pieces[hop], hop) for hop in (1, 2, 3)]

    cap = rows // 2
    each = cap // CHUNKS
    wide_row = model + NOTES

    def whole(shape):
        return pl.BlockSpec(shape, lambda k, where: (0, 0))

    def mine(k, where):
        return (where[3], 0)

    def hop_rows(k, where):
        return (where[3] ^ k, 0)

    out_shapes = [((rows, model), F32), ((GROUPS * cap, rows), BF16)]
    out_shapes += [((each, wide_row), BF16)] * (GROUPS * CHUNKS)
    updated, pick, *slots = pl.pallas_call(
        project_kernel,
        grid_spec=pltpu.PrefetchScalarGridSpec(
            num_scalar_prefetch=1,
            grid=(4,),
            in_specs=[whole((rows, 2 * width))] * 4
            + [pl.BlockSpec((width, model), hop_rows)] * 2
            + [whole((rows, model)), whole((1, model))]
            + [pl.BlockSpec((rows, 2), mine)] * 2,
            out_specs=[whole(s) for s, _ in out_shapes],
            scratch_shapes=[pltpu.VMEM((rows, model), F32)],
        ),
        out_shape=[jax.ShapeDtypeStruct(s, d) for s, d in out_shapes],
        compiler_params=pltpu.CompilerParams(
            vmem_limit_bytes=48 * 1024 * 1024, dimension_semantics=("arbitrary",)
        ),
        name="project",
    )(
        where, *pieces, broad_emission_proj, slim_emission_proj, skip_stream,
        premix_scaling_coeffs.reshape(1, model), routed_specialist_ids, routed_specialist_shares,
    )

    steps = 4
    hidden = specialist_valve_proj.shape[2]
    tile = 2 * hidden // steps
    rows_in = GROUPS * each

    def experts(*inputs):
        n = len(inputs)
        return call(
            functools.partial(expert_kernel, n),
            "experts",
            [((rows_in, model), BF16)] * n,
            [SMEM] + [VMEM] * n + [ANY] * 6,
            [
                pltpu.VMEM((steps, model, tile), BF16),
                pltpu.VMEM((steps, model, tile), BF16),
                pltpu.VMEM((steps, tile, model), BF16),
                pltpu.VMEM((n, rows_in, model), F32),
                pltpu.SemaphoreType.DMA((steps, 3)),
            ],
        )(where, *inputs, *sides)

    own, beside, across, corner = [], [], [], []
    for chunk in range(CHUNKS):
        sent = slots[chunk * GROUPS : (chunk + 1) * GROUPS]
        got = [sent[0]] + [turn_groups(sent[hop], hop) for hop in range(1, GROUPS)]
        own.append(jnp.concatenate(got, 0))
    for chunk in range(CHUNKS):
        beside.append(swap_expert(own[chunk]))
        across.append(swap_rows(own[chunk], 2))
    for chunk in range(CHUNKS):
        corner.append(
            swap_expert(across[chunk]) if chunk % 2 == 0 else swap_rows(beside[chunk], 2)
        )
    own = experts(*own)
    near = [experts(beside[chunk], across[chunk]) for chunk in range(CHUNKS)]
    corner = [experts(corner[chunk])[0] for chunk in range(CHUNKS)]
    back = []
    for chunk in range(CHUNKS):
        beside, across = near[chunk]
        if chunk % 2 == 0:
            across = (across.astype(F32) + swap_expert(corner[chunk]).astype(F32)).astype(BF16)
        else:
            beside = (beside.astype(F32) + swap_rows(corner[chunk], 2).astype(F32)).astype(BF16)
        total = (
            own[chunk].astype(F32)
            + swap_expert(beside).astype(F32)
            + swap_rows(across, 2).astype(F32)
        ).astype(BF16)
        back.append(total[:each])
        for hop in range(1, GROUPS):
            back.append(turn_groups(total[hop * each : (hop + 1) * each], GROUPS - hop))
    return call(
        combine_kernel, "combine", [((rows, model), BF16)], [VMEM] * (2 + GROUPS * CHUNKS)
    )(updated, pick, *back)[0]


def solution(mesh):
    sp, tp = mesh.shape["sp"], mesh.shape["tp"]
    paired = sp == 2 * GROUPS and tp == 4
    return jax.shard_map(
        functools.partial(paired_device, sp) if paired else general_device,
        mesh=mesh,
        in_specs=(
            P("sp", "tp"),
            P("sp", "tp"),
            P("sp", "tp"),
            P("sp", "tp"),
            P("sp", "tp"),
            P("sp", "tp"),
            P("sp", "tp"),
            P("sp", "tp"),
            P("tp"),
            P("tp"),
            P("tp"),
            P("tp"),
            P("sp"),
            P(),
            P(),
            P(("sp", "tp"), None),
            P(),
            P("sp", None),
            P("sp", None),
            P("sp", None, "tp"),
            P("sp", None, "tp"),
            P("sp", "tp", None),
        ),
        out_specs=P(("sp", "tp"), None),
        check_vma=False,
    )
```

```python
import functools

import jax
import jax.numpy as jnp
import numpy as np
from jax import lax
from jax.experimental import pallas as pl
from jax.experimental.pallas import tpu as pltpu
from jax.sharding import PartitionSpec as P

BROAD_CHANNEL_DIM = 128
THIN_CHANNEL_DIM = 64
GROUPS = 4


rope_base = 10000.0
epsilon = 1e-06


def entering(value, axis, join, neutral):
    place = lax.axis_index(axis)
    gathered = jax.tree.map(
        lambda a, kind: lax.all_gather(a.astype(kind), axis),
        value,
        (jnp.bfloat16, jnp.bfloat16, jnp.bfloat16, jnp.bfloat16),
    )
    state = jax.tree.map(lambda a, e: jnp.zeros_like(a) + jnp.asarray(e, a.dtype), value, neutral)

    def one(lap, state):
        return join(
            state,
            jax.tree.map(
                lambda a, own: lax.dynamic_index_in_dim(a, lap, 0, False).astype(own.dtype),
                gathered,
                value,
            ),
        )

    return lax.fori_loop(0, place, one, state)


def rotate(payload_tensor, positions):
    channel_dimension = payload_tensor.shape[-1]
    half = channel_dimension // 2
    freq = rope_base ** (-jnp.arange(half, dtype=jnp.float32) * 2.0 / channel_dimension)
    angle = positions.astype(jnp.float32)[:, None, None] * freq[None, None, :]
    cosine = jnp.cos(angle)
    sine = jnp.sin(angle)
    first = payload_tensor[..., :half]
    second = payload_tensor[..., half:]
    return jnp.concatenate([first * cosine - second * sine, first * sine + second * cosine], -1)


def segment_terms(probe_tensor, lookup_tensor, payload_tensor, surge_forgetting, forgetting_speed):
    length = probe_tensor.shape[0]
    segment_tally = jnp.arange(length, dtype=jnp.float32)
    memory_matrix = (
        forgetting_speed[None, :] * segment_tally[:, None] + jnp.cumsum(surge_forgetting)[:, None]
    )
    causal = (segment_tally[:, None] >= segment_tally[None, :])[None]
    level_t = jnp.transpose(memory_matrix)
    gap = level_t[:, :, None] - level_t[:, None, :]
    decay = jnp.where(causal, jnp.exp(jnp.where(causal, gap, 0.0)), 0.0)
    attention_scores = jnp.einsum(
        "szr,yzr->zsy", probe_tensor, lookup_tensor, preferred_element_type=jnp.float32
    )
    weights = (attention_scores * decay).astype(jnp.bfloat16)
    inner = jnp.einsum("htm,mhe->the", weights, payload_tensor, preferred_element_type=jnp.float32)
    factor = jnp.exp(memory_matrix + forgetting_speed[None, :])
    tail = jnp.exp(memory_matrix[-1:, :] - memory_matrix)
    weighted_output = (lookup_tensor.astype(jnp.float32) * tail[:, :, None]).astype(jnp.bfloat16)
    state_update = jnp.einsum(
        "oup,our->upr", weighted_output, payload_tensor, preferred_element_type=jnp.float32
    )
    total = jnp.exp(memory_matrix[-1] + forgetting_speed)
    return (inner, factor, state_update, total)


def read_state(probe_tensor, state):
    return jnp.einsum(
        "thd,hde->the", probe_tensor.astype(jnp.float32), state, precision=lax.Precision.HIGHEST
    )


def keeping_multiplier(
    probe_source,
    lookup_tensor,
    payload_tensor,
    forgetting_speed,
    surge_forgetting,
    channel_dimension,
    segment_begin,
):
    length = probe_source.shape[0]
    heads = probe_source.shape[1] // channel_dimension
    places = segment_begin + jnp.arange(length, dtype=jnp.int32)
    spun_probe = rotate(
        probe_source.astype(jnp.float32).reshape(length, heads, channel_dimension), places
    ).astype(jnp.bfloat16)
    spun_lookup = (
        rotate(lookup_tensor.astype(jnp.float32).reshape(length, heads, channel_dimension), places)
        * channel_dimension ** (-0.5)
    ).astype(jnp.bfloat16)
    regrouped_payload = payload_tensor.reshape(length, heads, channel_dimension)
    block = min(512, length)
    count = length // block

    def divider_mark(array):
        return array.reshape((count, block) + array.shape[1:])

    def segment_walker(carry, piece):
        state, prefix = carry
        block_q, block_k, block_v, block_b = piece
        inner, factor, state_update, total = segment_terms(
            block_q, block_k, block_v, block_b, forgetting_speed
        )
        local = inner + factor[:, :, None] * read_state(block_q, state)
        return (
            (total[:, None, None] * state + state_update, prefix * total),
            (local, factor * prefix[None, :]),
        )

    opening_location = (
        jnp.zeros((heads, channel_dimension, channel_dimension), jnp.float32),
        jnp.ones((heads,), jnp.float32),
    )
    (state, decay), (local, reach) = lax.scan(
        segment_walker,
        opening_location,
        (
            divider_mark(spun_probe),
            divider_mark(spun_lookup),
            divider_mark(regrouped_payload),
            divider_mark(surge_forgetting),
        ),
    )
    return (
        spun_probe,
        local.reshape(length, heads, channel_dimension),
        reach.reshape(length, heads),
        decay,
        state,
    )


def finish(sublayer_final, emission_valve, scaling_coefficients):
    length, heads, channel_dimension = sublayer_final.shape
    normed = sublayer_final * lax.rsqrt(
        jnp.mean(sublayer_final * sublayer_final, -1, keepdims=True) + epsilon
    )
    gated = (
        normed.reshape(length, heads * channel_dimension)
        * scaling_coefficients[None, :]
        * jax.nn.silu(emission_valve.astype(jnp.float32))
    )
    return gated.astype(jnp.bfloat16)


def chain(earlier, later):
    return (
        earlier[0] * later[0],
        later[0][:, None, None] * earlier[1] + later[1],
        earlier[2] * later[2],
        later[2][:, None, None] * earlier[3] + later[3],
    )


def slot_positions(chosen, experts, cap):
    listed = chosen.reshape(-1)
    matches = (listed[:, None] == jnp.arange(experts, dtype=jnp.int32)[None, :]).astype(jnp.int32)
    before = jnp.cumsum(matches, 0) - matches
    order = jnp.sum(before * matches, 1)
    return (listed * cap + order).reshape(chosen.shape)


def fill_slots(rows_in, chosen, experts, cap):
    count = rows_in.shape[0]
    places = slot_positions(chosen, experts, cap).reshape(-1)
    owners = jnp.repeat(jnp.arange(count, dtype=jnp.int32), 2)
    source = jnp.full((experts * cap,), count, jnp.int32).at[places].set(owners)
    padded = jnp.concatenate([rows_in, jnp.zeros((1, rows_in.shape[1]), rows_in.dtype)], 0)
    return padded[source].reshape(experts, cap, rows_in.shape[1])


def general_device(
    broad_probe_tensor,
    broad_lookup_tensor,
    broad_payload_tensor,
    broad_emission_valve,
    slim_probe_tensor,
    slim_lookup_tensor,
    slim_payload_tensor,
    slim_emission_valve,
    broad_forgetting_speed,
    slim_forgetting_speed,
    broad_channel_scaling,
    slim_channel_scaling,
    surge_forgetting,
    broad_emission_proj,
    slim_emission_proj,
    skip_stream,
    premix_scaling_coeffs,
    routed_specialist_ids,
    routed_specialist_shares,
    specialist_valve_proj,
    specialist_expand_proj,
    specialist_contract_proj,
):
    length = broad_probe_tensor.shape[0]
    segment_begin = lax.axis_index("sp") * length
    wide_result = keeping_multiplier(
        broad_probe_tensor,
        broad_lookup_tensor,
        broad_payload_tensor,
        broad_forgetting_speed,
        surge_forgetting,
        BROAD_CHANNEL_DIM,
        segment_begin,
    )
    narrow_result = keeping_multiplier(
        slim_probe_tensor,
        slim_lookup_tensor,
        slim_payload_tensor,
        slim_forgetting_speed,
        surge_forgetting,
        THIN_CHANNEL_DIM,
        segment_begin,
    )
    identity = (
        jnp.ones_like(wide_result[3]),
        jnp.zeros_like(wide_result[4]),
        jnp.ones_like(narrow_result[3]),
        jnp.zeros_like(narrow_result[4]),
    )
    incoming = entering(
        (wide_result[3], wide_result[4], narrow_result[3], narrow_result[4]), "sp", chain, identity
    )
    mixed_wide = finish(
        wide_result[1] + wide_result[2][:, :, None] * read_state(wide_result[0], incoming[1]),
        broad_emission_valve,
        broad_channel_scaling,
    )
    mixed_narrow = finish(
        narrow_result[1] + narrow_result[2][:, :, None] * read_state(narrow_result[0], incoming[3]),
        slim_emission_valve,
        slim_channel_scaling,
    )
    rows_wide, rows_narrow = (
        lax.all_to_all(mixed_wide, "tp", split_axis=0, concat_axis=1, tiled=True),
        lax.all_to_all(mixed_narrow, "tp", split_axis=0, concat_axis=1, tiled=True),
    )
    projected = jnp.dot(rows_wide, broad_emission_proj, preferred_element_type=jnp.float32)
    projected = projected + jnp.dot(
        rows_narrow, slim_emission_proj, preferred_element_type=jnp.float32
    )
    updated = skip_stream.astype(jnp.float32) + projected
    scale = lax.rsqrt(jnp.mean(updated * updated, -1, keepdims=True) + epsilon)
    normed = (updated * scale * premix_scaling_coeffs[None, :]).astype(jnp.bfloat16)
    rows = normed.shape[0]
    width = normed.shape[1]
    experts = lax.axis_size("sp") * specialist_valve_proj.shape[0]
    cap = rows * GROUPS // experts
    own_ids = lax.dynamic_slice_in_dim(routed_specialist_ids, lax.axis_index("tp") * rows, rows, 0)
    own_weights = lax.dynamic_slice_in_dim(
        routed_specialist_shares, lax.axis_index("tp") * rows, rows, 0
    )
    own_places = slot_positions(own_ids, experts, cap)
    sent = lax.all_to_all(
        fill_slots(normed, own_ids, experts, cap), "sp", split_axis=0, concat_axis=0, tiled=True
    )
    arrived = lax.all_gather(sent, "tp", axis=0, tiled=True)
    slots = arrived.reshape(-1, width)
    emission_valve = jnp.dot(slots, specialist_valve_proj[0], preferred_element_type=jnp.float32)
    up = jnp.dot(slots, specialist_expand_proj[0], preferred_element_type=jnp.float32)
    hidden = (jax.nn.silu(emission_valve) * up).astype(jnp.bfloat16)
    summed = lax.psum_scatter(
        jnp.dot(hidden, specialist_contract_proj[0], preferred_element_type=jnp.float32).astype(
            jnp.bfloat16
        ),
        "tp",
        scatter_dimension=0,
        tiled=True,
    )
    expert_out = summed.reshape(experts, cap, width)
    returned = lax.all_to_all(expert_out, "sp", split_axis=0, concat_axis=0, tiled=True)
    picked = returned.reshape(experts * cap, width)[own_places]
    mixture = jnp.sum(own_weights[:, :, None] * picked.astype(jnp.float32), 1)
    return (updated + mixture).astype(jnp.bfloat16)


LANES = 128
NOTES = 128
F32 = jnp.float32
BF16 = jnp.bfloat16


FINE = 32


def rope_tables(length, blocks):
    fine, coarse = [], []
    for dim in (BROAD_CHANNEL_DIM, THIN_CHANNEL_DIM):
        lane = np.arange(LANES) % dim
        freq = rope_base ** (-(lane % (dim // 2)) * 2.0 / dim)
        sign = np.where(lane < dim // 2, -1.0, 1.0)
        for rows, step, into in ((FINE, 1, fine), (length * blocks // FINE, FINE, coarse)):
            angle = np.arange(rows)[:, None] * step * freq[None, :]
            into += [np.cos(angle), np.sin(angle) * sign]
    return np.stack(fine).astype(np.float32), np.stack(coarse).astype(np.float32)


def swap_halves(x, group):
    if group == 0:
        return pltpu.roll(x, 64, 1)
    lane = lax.broadcasted_iota(jnp.int32, x.shape, 1)
    return jnp.where(lane % 64 < 32, pltpu.roll(x, 96, 1), pltpu.roll(x, 32, 1))


def running_sum(surge_ref):
    length = surge_ref.shape[1]
    row = jnp.broadcast_to(surge_ref[...], (8, length))
    lane = lax.broadcasted_iota(jnp.int32, row.shape, 1)
    step = 1
    while step < length:
        row = row + jnp.where(lane >= step, pltpu.roll(row, step, 1), 0.0)
        step *= 2
    return row[0:1, :]


def as_column(row):
    length = row.shape[1]
    t = lax.broadcasted_iota(jnp.int32, (length, length), 0)
    m = lax.broadcasted_iota(jnp.int32, (length, length), 1)
    return jnp.sum(jnp.where(t == m, row, jnp.zeros_like(row)), axis=1, keepdims=True)


def low_half(shape):
    return lax.broadcasted_iota(jnp.int32, shape, 1) < 64


def dot(a, b, dims=((1,), (0,))):
    return lax.dot_general(a, b, (dims, ((), ())), preferred_element_type=F32)


def increment_kernel(
    where_ref, wide_rate_in, slim_rate_in, surge_in, fine_in, coarse_in,
    kw_in, vw_in, kn_in, vn_in,
    kw_out, kn_out, message_ref, turn_ref, column_ref, row_ref, rate_ref,
    wide_rate, slim_rate, surge_ref, fine_ref, coarse_ref, kw_ref, vw_ref, kn_ref, vn_ref, sems,
):
    length = kw_ref.shape[0]
    parts = length // FINE
    copies = [
        pltpu.make_async_copy(source, target, sems.at[i])
        for i, (source, target) in enumerate(
            (
                (wide_rate_in, wide_rate),
                (slim_rate_in, slim_rate),
                (surge_in, surge_ref),
                (fine_in, fine_ref),
                (coarse_in.at[:, pl.ds(where_ref[0] * parts, parts), :], coarse_ref),
                (kw_in, kw_ref),
                (vw_in, vw_ref),
                (kn_in, kn_ref),
                (vn_in, vn_ref),
            )
        )
    ]
    for copy in copies:
        copy.start()
    for copy in copies[:5]:
        copy.wait()
    row = running_sum(surge_ref)
    column = as_column(row)
    column_ref[...] = jnp.broadcast_to(column, (length, LANES))
    row_ref[...] = jnp.broadcast_to(row, row_ref.shape)
    for i in range(2):
        rate_ref[i : i + 1, :] = jnp.full((1, LANES), wide_rate[i])
    for i in range(4):
        rate_ref[i + 2 : i + 3, :] = jnp.full((1, LANES), slim_rate[i])
    for group in range(2):
        ci, si = fine_ref[2 * group], fine_ref[2 * group + 1]
        for part in range(parts):
            cb = coarse_ref[2 * group, part : part + 1, :]
            sb = coarse_ref[2 * group + 1, part : part + 1, :]
            rows = slice(part * FINE, (part + 1) * FINE)
            turn_ref[2 * group, rows, :] = ci * cb - si * sb
            turn_ref[2 * group + 1, rows, :] = si * cb + ci * sb
    last = row[0:1, length - 1 : length]
    offset = lax.broadcasted_iota(jnp.int32, (length, 1), 0).astype(F32)
    back = (length - 1.0) - offset
    below = last - column
    half = low_half((1, LANES))
    decays = []
    for copy in copies[5:]:
        copy.wait()
    for group, (k_ref, v_ref, k_out, rates) in enumerate(
        ((kw_ref, vw_ref, kw_out, wide_rate), (kn_ref, vn_ref, kn_out, slim_rate))
    ):
        cosine, sine = turn_ref[2 * group], turn_ref[2 * group + 1]
        scale = (BROAD_CHANNEL_DIM, THIN_CHANNEL_DIM)[group] ** -0.5
        for slot in range(2):
            cols = slice(slot * LANES, (slot + 1) * LANES)
            k = k_ref[:, cols].astype(F32)
            spun = ((k * cosine + swap_halves(k, group) * sine) * scale).astype(BF16)
            k_out[:, cols] = spun
            if group == 0:
                tail = jnp.exp(rates[slot] * back + below)
                decay = jnp.exp(jnp.full((1, LANES), rates[slot] * length) + last)
            else:
                a, b = rates[2 * slot], rates[2 * slot + 1]
                tail = jnp.where(half, jnp.exp(a * back + below), jnp.exp(b * back + below))
                decay = jnp.exp(jnp.where(half, a * length, b * length) + last)
            weighted = (spun.astype(F32) * tail).astype(BF16)
            gain = dot(weighted, v_ref[:, cols], ((0,), (0,)))
            if group == 1:
                upper = lax.broadcasted_iota(jnp.int32, (LANES, LANES), 0) < 64
                gain = jnp.where(upper == low_half((LANES, LANES)), gain, 0.0)
            place = (2 * group + slot) * LANES
            message_ref[place : place + LANES, :] = gain.astype(BF16)
            decays.append(decay)
    high = [d.astype(BF16).astype(F32) for d in decays]
    low = [d - h for d, h in zip(decays, high)]
    notes = jnp.concatenate(high + low + [jnp.zeros((8, LANES), F32)], 0)
    message_ref[4 * LANES :, :] = notes.astype(BF16)


def unpack(ref):
    notes = ref[4 * LANES :, :].astype(F32)
    decays = [notes[i : i + 1] + notes[i + 4 : i + 5] for i in range(4)]
    states = [ref[i * LANES : (i + 1) * LANES, :].astype(F32) for i in range(4)]
    return states, decays


def pair_kernel(where_ref, own_ref, other_ref, out_ref):
    late = where_ref[2] == 1
    own, own_decay = unpack(own_ref)
    other, other_decay = unpack(other_ref)
    high, low = [], []
    for i in range(4):
        first = jnp.where(late, other[i], own[i])
        second = jnp.where(late, own[i], other[i])
        decay = jnp.where(late, own_decay[i], other_decay[i])
        out_ref[i * LANES : (i + 1) * LANES, :] = (decay * first + second).astype(BF16)
        both = own_decay[i] * other_decay[i]
        high.append(both.astype(BF16).astype(F32))
        low.append(both - high[-1])
    notes = jnp.concatenate(high + low + [jnp.zeros((8, LANES), F32)], 0)
    out_ref[4 * LANES :, :] = notes.astype(BF16)


def inner_kernel(group, turn_ref, column_ref, row_ref, rate_ref, q_ref, k_ref, v_ref, q_out, out):
    length = q_ref.shape[0]
    cosine, sine = turn_ref[2 * group], turn_ref[2 * group + 1]
    for slot in range(2):
        cols = slice(slot * LANES, (slot + 1) * LANES)
        q = q_ref[:, cols].astype(F32)
        q_out[:, cols] = (q * cosine + swap_halves(q, group) * sine).astype(BF16)
    tile = min(128, length)
    half = low_half((tile, LANES))
    for block in range(length // tile):
        begin, n = block * tile, (block + 1) * tile
        rows = slice(begin, n)
        t = lax.broadcasted_iota(jnp.int32, (tile, n), 0) + begin
        m = lax.broadcasted_iota(jnp.int32, (tile, n), 1)
        causal = t >= m
        apart = (t - m).astype(F32)
        fall = column_ref[rows, 0:1] - row_ref[0:1, :n]

        def mixed(q, k, v, head):
            decay = jnp.where(causal, jnp.exp(rate_ref[head : head + 1, 0:1] * apart + fall), 0.0)
            return dot((dot(q, k, ((1,), (1,))) * decay).astype(BF16), v)

        for slot in range(2):
            cols = slice(slot * LANES, (slot + 1) * LANES)
            q, k, v = q_out[rows, cols], k_ref[:n, cols], v_ref[:n, cols]
            if group == 0:
                out[rows, cols] = mixed(q, k, v, slot)
            else:
                nothing = jnp.zeros_like(q)
                first = mixed(jnp.where(half, q, nothing), k, v, 2 + 2 * slot)
                second = mixed(jnp.where(half, nothing, q), k, v, 3 + 2 * slot)
                out[rows, cols] = jnp.where(half, first, second)


def finish_kernel(
    hops, where_ref, rate_ref, column_ref, wide_q, slim_q, wide_inner, slim_inner,
    other_ref, near_ref, mid_ref, far_ref,
    wide_gate, slim_gate, wide_gain, slim_gain,
    *outs,
):
    late = where_ref[2] == 1
    tp_index = where_ref[3]
    rows = outs[0].shape[0]
    near, near_decay = unpack(near_ref)
    mid, mid_decay = unpack(mid_ref)
    far, _ = unpack(far_ref)
    other, other_decay = unpack(other_ref)
    states = []
    for i in range(4):
        state = near[i] + near_decay[i] * (mid[i] + mid_decay[i] * far[i])
        state = jnp.where(late, other_decay[i] * state + other[i], state)
        high = state.astype(BF16)
        states.append((high, (state - high.astype(F32)).astype(BF16)))
    half = low_half((rows, LANES))
    for hop, out in zip(hops, outs):
        begin = pl.multiple_of((tp_index ^ hop) * rows, rows)
        at = pl.ds(begin, rows)
        column = column_ref[at, :]
        offset = (lax.broadcasted_iota(jnp.int32, (rows, LANES), 0) + begin + 1).astype(F32)
        for i in range(4):
            cols = slice(i * LANES, (i + 1) * LANES)
            part = slice((i % 2) * LANES, (i % 2 + 1) * LANES)
            if i < 2:
                q_ref, inner_ref, gate_ref, gain_ref = wide_q, wide_inner, wide_gate, wide_gain
                rate = rate_ref[i : i + 1, :]
            else:
                q_ref, inner_ref, gate_ref, gain_ref = slim_q, slim_inner, slim_gate, slim_gain
                rate = jnp.where(
                    half, rate_ref[2 * i - 2 : 2 * i - 1, :], rate_ref[2 * i - 1 : 2 * i, :]
                )
            q = q_ref[at, part]
            read = dot(q, states[i][0]) + dot(q, states[i][1])
            factor = jnp.exp(rate * offset + column)
            value = inner_ref[at, part] + factor * read
            square = value * value
            if i < 2:
                mean = jnp.mean(square, axis=1, keepdims=True)
            else:
                first = jnp.sum(jnp.where(half, square, 0.0), axis=1, keepdims=True)
                second = jnp.sum(jnp.where(half, 0.0, square), axis=1, keepdims=True)
                mean = jnp.where(half, first, second) / THIN_CHANNEL_DIM
            gate = gate_ref[at, part].astype(F32)
            value = value * lax.rsqrt(mean + epsilon) * gain_ref[:, part]
            out[:, cols] = (value * (gate / (1.0 + jnp.exp(-gate)))).astype(BF16)


def project_near_kernel(
    where_ref, p0, p1, wide_ref, slim_ref, skip_ref, sum_ref, rest_ref, buffer, sems
):
    width = p0.shape[1] // 2
    copies = []
    for hop in range(4):
        at = pl.ds(pl.multiple_of((where_ref[3] ^ hop) * width, width), width)
        for i, source in enumerate((wide_ref, slim_ref)):
            span = slice(i * width, (i + 1) * width)
            target = buffer.at[hop, span, :] if hop < 2 else rest_ref.at[hop - 2, span, :]
            copies.append(pltpu.make_async_copy(source.at[at, :], target, sems.at[hop, i]))
    for copy in copies:
        copy.start()
    total = skip_ref[...].astype(F32)
    for hop, piece in enumerate((p0, p1)):
        copies[2 * hop].wait()
        copies[2 * hop + 1].wait()
        total += dot(piece[...], buffer[hop])
    sum_ref[...] = total
    for copy in copies[4:]:
        copy.wait()


def project_far_kernel(
    where_ref, sum_ref, rest_ref, p2, p3, gain_ref, ids_ref, shares_ref,
    updated_ref, pick_ref, *outs,
):
    rows = p2.shape[0]
    updated = sum_ref[...] + dot(p2[...], rest_ref[0]) + dot(p3[...], rest_ref[1])
    own = pl.ds(pl.multiple_of(where_ref[3] * rows, rows), rows)
    updated_ref[...] = updated
    scale = lax.rsqrt(jnp.mean(updated * updated, axis=1, keepdims=True) + epsilon)
    normed = (updated * scale * gain_ref[...]).astype(BF16)
    ids, shares = ids_ref[own, :], shares_ref[own, :]
    first, second = ids[:, 0:1], ids[:, 1:2]
    group = first // 2
    straight = first < second
    low = jnp.where(straight, shares[:, 0:1], shares[:, 1:2])
    high = jnp.where(straight, shares[:, 1:2], shares[:, 0:1])
    lane = lax.broadcasted_iota(jnp.int32, (rows, NOTES), 1)
    share = jnp.where(lane < 2, low, high)
    top = share.astype(BF16).astype(F32)
    notes = jnp.where(lane % 2 == 0, top, share - top).astype(BF16)
    t = lax.broadcasted_iota(jnp.int32, (rows, rows), 0)
    m = lax.broadcasted_iota(jnp.int32, (rows, rows), 1)
    group_f = jnp.broadcast_to(group.astype(F32), (rows, rows))
    across = jnp.sum(jnp.where(t == m, group_f, 0.0), axis=0, keepdims=True)
    ahead = jnp.where((group_f == across) & (t < m), 1.0, 0.0)
    order = jnp.sum(ahead, axis=0, keepdims=True).astype(jnp.int32)
    across = across.astype(jnp.int32)
    cap = pick_ref.shape[0] // GROUPS
    slot = lax.broadcasted_iota(jnp.int32, (cap, rows), 0)
    for hop in range(GROUPS):
        aim = (where_ref[1] + hop) % GROUPS
        pick = jnp.where((order == slot) & (across == aim), 1.0, 0.0).astype(BF16)
        pick_ref[hop * cap : (hop + 1) * cap, :] = pick
        body = dot(pick, normed).astype(BF16)
        side = dot(pick, notes).astype(BF16)
        outs[hop][:, : normed.shape[1]] = body
        outs[hop][:, normed.shape[1] :] = side


def expert_kernel(count, where_ref, *refs):
    blocks = refs[:count]
    weights = refs[count : count + 6]
    outs = refs[count + 6 : 2 * count + 6]
    x_ref = refs[2 * count + 6]
    rows, model = outs[0].shape
    shares = []
    late = where_ref[2] == 1
    for i, block in enumerate(blocks):
        x_ref[i * rows : (i + 1) * rows, :] = block[:, :model]
        notes = block[:, model : model + 4].astype(F32)
        shares.append(
            jnp.where(late, notes[:, 2:3] + notes[:, 3:4], notes[:, 0:1] + notes[:, 1:2])
        )
    total = None
    for side in range(2):
        gate = dot(x_ref[...], weights[side][0])
        up = dot(x_ref[...], weights[2 + side][0])
        hidden = (gate / (1.0 + jnp.exp(-gate)) * up).astype(BF16)
        part = dot(hidden, weights[4 + side][0])
        total = part if total is None else total + part
    for i in range(count):
        outs[i][...] = (total[i * rows : (i + 1) * rows] * shares[i]).astype(BF16)


def combine_kernel(updated_ref, pick_ref, *refs):
    parts, out = refs[:-1], refs[-1]
    cap = parts[0].shape[0]
    total = updated_ref[...]
    for hop, part in enumerate(parts):
        total = total + dot(pick_ref[hop * cap : (hop + 1) * cap, :], part[...], ((0,), (0,)))
    out[...] = total.astype(BF16)


SMEM = pl.BlockSpec(memory_space=pltpu.SMEM)
VMEM = pl.BlockSpec(memory_space=pltpu.VMEM)
HBM = pl.BlockSpec(memory_space=pltpu.MemorySpace.HBM)
BIG = pltpu.CompilerParams(vmem_limit_bytes=20 * 1024 * 1024)


def in_hbm(a):
    return pltpu.with_memory_space_constraint(a, pltpu.MemorySpace.HBM)


def call(kernel, outs, specs, scratch=(), flops=0):
    shapes = [jax.ShapeDtypeStruct(s, d) for s, d in outs]
    return pl.pallas_call(
        kernel,
        out_shape=shapes,
        in_specs=specs,
        out_specs=[VMEM] * len(shapes),
        scratch_shapes=list(scratch),
        compiler_params=BIG,
        cost_estimate=pl.CostEstimate(flops=flops, bytes_accessed=0, transcendentals=0),
    )


def paired_device(
    blocks,
    broad_probe_tensor,
    broad_lookup_tensor,
    broad_payload_tensor,
    broad_emission_valve,
    slim_probe_tensor,
    slim_lookup_tensor,
    slim_payload_tensor,
    slim_emission_valve,
    broad_forgetting_speed,
    slim_forgetting_speed,
    broad_channel_scaling,
    slim_channel_scaling,
    surge_forgetting,
    broad_emission_proj,
    slim_emission_proj,
    skip_stream,
    premix_scaling_coeffs,
    routed_specialist_ids,
    routed_specialist_shares,
    specialist_valve_proj,
    specialist_expand_proj,
    specialist_contract_proj,
):
    length, width = broad_probe_tensor.shape
    rows, model = skip_stream.shape
    sp_index, tp_index = lax.axis_index("sp"), lax.axis_index("tp")
    where = jnp.stack([sp_index, sp_index // 2, sp_index % 2, tp_index]).astype(jnp.int32)

    def swap_expert(a):
        return lax.ppermute(a, "sp", [(i, i ^ 1) for i in range(blocks)])

    def swap_rows(a, hop):
        return lax.ppermute(a, "tp", [(i, i ^ hop) for i in range(4)])

    def turn_groups(a, hop):
        return lax.ppermute(a, "sp", [(i, (i + 2 * hop) % blocks) for i in range(blocks)])

    def pass_on(a, hop):
        return lax.ppermute(a, "sp", [(i, i + 2 * hop) for i in range(blocks - 2 * hop)])

    sides = []
    for w in (specialist_valve_proj, specialist_expand_proj, specialist_contract_proj):
        sides += [w, swap_rows(w, 1)]

    fine, coarse = rope_tables(length, blocks)
    parts = coarse.shape[1] // blocks
    spun_wide, spun_slim, message, turn, column, row, rates = call(
        increment_kernel,
        [
            ((length, width), BF16),
            ((length, width), BF16),
            ((4 * LANES + 16, LANES), BF16),
            ((4, length, LANES), F32),
            ((length, LANES), F32),
            ((8, length), F32),
            ((8, LANES), F32),
        ],
        [SMEM] + [HBM] * 9,
        [
            pltpu.SMEM(broad_forgetting_speed.shape, F32),
            pltpu.SMEM(slim_forgetting_speed.shape, F32),
            pltpu.VMEM((1, length), F32),
            pltpu.VMEM(fine.shape, F32),
            pltpu.VMEM((4, parts, LANES), F32),
        ]
        + [pltpu.VMEM((length, width), BF16)] * 4
        + [pltpu.SemaphoreType.DMA((9,))],
        flops=10**9,
    )(
        where,
        *map(
            in_hbm,
            (
                broad_forgetting_speed, slim_forgetting_speed, surge_forgetting.reshape(1, length),
                jnp.asarray(fine), jnp.asarray(coarse),
                broad_lookup_tensor, broad_payload_tensor, slim_lookup_tensor, slim_payload_tensor,
            ),
        ),
    )
    other = swap_expert(message)
    pair = call(pair_kernel, [(message.shape, BF16)], [SMEM] + [VMEM] * 2)(where, message, other)[0]
    passed = []
    for hop in range(1, GROUPS):
        passed.append(pass_on(pair, hop))

    def inner(group, *inputs):
        return call(
            functools.partial(inner_kernel, group),
            [((length, width), BF16), ((length, width), F32)],
            [VMEM] * 7,
            flops=2 * 10**9,
        )(turn, column, row, rates, *inputs)

    wide_q, wide_inner = inner(0, broad_probe_tensor, spun_wide, broad_payload_tensor)
    slim_q, slim_inner = inner(1, slim_probe_tensor, spun_slim, slim_payload_tensor)

    def finish(hops):
        return call(
            functools.partial(finish_kernel, hops),
            [((rows, 2 * width), BF16)] * len(hops),
            [SMEM] + [VMEM] * 14,
            flops=10**9,
        )(
            where, rates, column, wide_q, slim_q, wide_inner, slim_inner, other, *passed,
            broad_emission_valve, slim_emission_valve,
            broad_channel_scaling.reshape(1, width), slim_channel_scaling.reshape(1, width),
        )

    cap = rows // 2
    p2, p3 = finish((2, 3))
    p0, p1 = finish((0, 1))
    p1, p2, p3 = (swap_rows(p, hop) for hop, p in ((1, p1), (2, p2), (3, p3)))
    partial_sum, rest = call(
        project_near_kernel,
        [((rows, model), F32), ((2, 2 * width, model), BF16)],
        [SMEM] + [VMEM] * 2 + [HBM] * 2 + [VMEM],
        [pltpu.VMEM((2, 2 * width, model), BF16), pltpu.SemaphoreType.DMA((4, 2))],
        flops=2 * 10**9,
    )(where, p0, p1, in_hbm(broad_emission_proj), in_hbm(slim_emission_proj), skip_stream)
    updated, pick, *slots = call(
        project_far_kernel,
        [((rows, model), F32), ((GROUPS * cap, rows), BF16)]
        + [((cap, model + NOTES), BF16)] * GROUPS,
        [SMEM] + [VMEM] * 7,
        flops=2 * 10**9,
    )(
        where, partial_sum, rest, p2, p3,
        premix_scaling_coeffs.reshape(1, model), routed_specialist_ids, routed_specialist_shares,
    )

    def experts(*inputs):
        n = len(inputs)
        return call(
            functools.partial(expert_kernel, n),
            [((cap, model), BF16)] * n,
            [SMEM] + [VMEM] * (n + 6),
            [pltpu.VMEM((n * cap, model), BF16)],
            flops=3 * 10**9,
        )(where, *inputs, *sides)

    hops = range(GROUPS)
    odd = [hop % 2 == 1 for hop in hops]
    own = [slots[0]]
    for hop in hops[1:]:
        own.append(turn_groups(slots[hop], hop))
    beside = [swap_expert(own[hop]) for hop in hops]
    across = [swap_rows(own[hop], 2) for hop in hops]
    corner = [swap_expert(across[hop]) if odd[hop] else swap_rows(beside[hop], 2) for hop in hops]
    mine, far = [None] * GROUPS, [None] * GROUPS
    left, up = [None] * GROUPS, [None] * GROUPS
    mine[0], mine[1], left[0], up[0] = experts(own[0], own[1], beside[0], across[0])
    mine[2], mine[3], left[1], up[1] = experts(own[2], own[3], beside[1], across[1])
    left[2], up[2], far[1] = experts(beside[2], across[2], corner[1])
    left[3], up[3], far[2] = experts(beside[3], across[3], corner[2])
    far[3], far[0] = experts(corner[3], corner[0])
    back = []
    for hop in hops:
        beside, across = left[hop], up[hop]
        if odd[hop]:
            came = swap_expert(far[hop])
            across = (across.astype(F32) + came.astype(F32)).astype(BF16)
        else:
            came = swap_rows(far[hop], 2)
            beside = (beside.astype(F32) + came.astype(F32)).astype(BF16)
        total = (
            mine[hop].astype(F32)
            + swap_expert(beside).astype(F32)
            + swap_rows(across, 2).astype(F32)
        ).astype(BF16)
        back.append(turn_groups(total, GROUPS - hop) if hop else total)
    return call(combine_kernel, [((rows, model), BF16)], [VMEM] * (2 + GROUPS))(
        updated, pick, *back
    )[0]


def solution(mesh):
    sp, tp = mesh.shape["sp"], mesh.shape["tp"]
    paired = sp == 2 * GROUPS and tp == 4

    def device(*inputs):
        if not paired:
            return general_device(*inputs)
        return paired_device(sp, *inputs)

    return jax.shard_map(
        device,
        mesh=mesh,
        in_specs=(
            P("sp", "tp"),
            P("sp", "tp"),
            P("sp", "tp"),
            P("sp", "tp"),
            P("sp", "tp"),
            P("sp", "tp"),
            P("sp", "tp"),
            P("sp", "tp"),
            P("tp"),
            P("tp"),
            P("tp"),
            P("tp"),
            P("sp"),
            P(),
            P(),
            P(("sp", "tp"), None),
            P(),
            P("sp", None),
            P("sp", None),
            P("sp", None, "tp"),
            P("sp", None, "tp"),
            P("sp", "tp", None),
        ),
        out_specs=P(("sp", "tp"), None),
        check_vma=False,
    )
```
